256 devices in a mesh: ep: 64 (over z, y, core), tp: 4 (over x).
Axes of the slice: x: 4, y: 4, z: 8, core: 2. Of those that a mesh axis runs over, the one named last changes fastest.
Arguments:
- mixer_in: bfloat16 [24576, 2048], P(('ep', 'tp')), may hold values from -8192 to 8192
- mixer_gain: float32 [2048], replicated, may hold values from 0.1 to 1.9
- query_weight: bfloat16 [2048, 512], P(None, 'tp'), may hold values from -4 to 4
- key_weight: bfloat16 [2048, 512], P(None, 'tp'), may hold values from -4 to 4
- value_weight: bfloat16 [2048, 512], P(None, 'tp'), may hold values from -0.125 to 0.125
- head_lambda: float32 [4], P('tp'), may hold values from 0.3 to 0.8
- head_gain: float32 [128], replicated, may hold values from 0.1 to 1.9
- out_weight: bfloat16 [512, 2048], P('tp'), may hold values from -0.25 to 0.25
- expert_in: bfloat16 [24576, 2048], P(('ep', 'tp')), may hold values from -6 to 6
- expert_gain: float32 [2048], replicated, may hold values from 0.1 to 1.9
- routes: int32 [24576, 2], P(('ep', 'tp')), may hold values from 0 to 63, all different within a row; in each aligned block of 96 rows (0 to 95, 96 to 191, ...) at most 6 rows name the same one
- route_weights: float32 [24576, 2], P(('ep', 'tp')), may hold values from 0.1 to 1
- gate_weight: bfloat16 [64, 2048, 512], P('ep'), may hold values from -0.125 to 0.125
- up_weight: bfloat16 [64, 2048, 512], P('ep'), may hold values from -0.125 to 0.125
- down_weight: bfloat16 [64, 512, 2048], P('ep'), may hold values from -0.25 to 0.25
- shared_gate: bfloat16 [2048, 512], P(None, 'tp'), may hold values from -0.125 to 0.125
- shared_up: bfloat16 [2048, 512], P(None, 'tp'), may hold values from -0.125 to 0.125
- shared_down: bfloat16 [512, 2048], P('tp'), may hold values from -0.25 to 0.25
Outputs:
- mixed_out: bfloat16 [24576, 2048], P(('ep', 'tp'))
- expert_out: bfloat16 [24576, 2048], P(('ep', 'tp'))
The draws below stay inside these ranges and needn't reach their ends.
Inputs may be any that keep to these rules, and one draw needn't show every extreme that they name: `routes`: each row names 2 different experts. Among the 96 rows of one device no expert is named more than 6 times, and in every draw some device's rows name some expert exactly 6 times.
All inputs are finite; a program needn't handle non-finite values.
Results may differ from the reference program's by a relative error of at most 0.013.
The reference program's roundings to bfloat16 on the way count: a program that leaves them out, or rounds other values in their place, can miss the bound.
Values may be sent and summed in bfloat16 or wider, within the bound.
No kernel may reach another device: no remote copies, remote signals or barrier semaphores. Data moves between devices by JAX's collectives and lax.ppermute only.
A program may use at most 128 MiB of HBM per device.

```python
import math
from functools import partial
import jax
import jax.numpy as jnp
import numpy as np
from jax import lax

D = 2048
HEADS = 4
HALF = 64
VDIM = 128
FE = 512
FS = 512
TOPK = 2
TOK_DEV = 96
TOKENS = 24576
EXPERTS = 64
CAP = 6
N_TP = 4


def draw_mixer_in(key, part):
    key_base = jax.random.fold_in(jax.random.fold_in(key, 31), 0)
    base = jnp.clip(jax.random.normal(key_base, (TOKENS, D), jnp.float32), -6.0, 6.0)
    return base.astype(jnp.bfloat16)


def draw_query_weight(key, part):
    normal_part = jax.random.normal(jax.random.fold_in(key, 21), (D, HEADS * 2 * HALF), jnp.float32)
    base = jnp.clip(normal_part, -4.0, 4.0) * math.sqrt(3.0 / D)
    return base.astype(jnp.bfloat16)


def draw_key_weight(key, part):
    normal_part = jax.random.normal(jax.random.fold_in(key, 22), (D, HEADS * 2 * HALF), jnp.float32)
    base = jnp.clip(normal_part, -4.0, 4.0) * math.sqrt(1.0 / D)
    return base.astype(jnp.bfloat16)


def steps_of(stream_key, dims, pieces, low, largest):
    factor_of, own = 1.0, jax.random.fold_in(stream_key, 6)
    for dim, shards_of in pieces:
        draws = jnp.exp(jax.random.uniform(jax.random.fold_in(own, dim), (shards_of,), jnp.float32, low / len(pieces), largest / len(pieces)))
        factor_of = factor_of * jnp.repeat(draws, dims[dim] // shards_of).reshape([-1 if axis == dim else 1 for axis in range(len(dims))])
    return factor_of


def assign_block(stream_key, own, number, rows, amount, top, limit, slope):
    sequence = jax.random.permutation(stream_key, amount)
    crowded, common = load_shares(amount, rows * top, limit, slope, True), load_shares(amount, rows * top, limit, slope, False)
    places = jnp.arange(amount)

    def named(sizes, turn):
        used = int((sizes > 0).sum())
        fixed = max(1, used // 4)
        passed = fixed + (places - fixed + turn * (used - fixed)) % max(1, amount - fixed)
        return jnp.zeros((amount,), jnp.int32).at[sequence[jnp.where(places < fixed, places, passed)]].set(jnp.asarray(sizes, jnp.int32))

    sizes = jnp.where(number % 4 == 0, named(crowded, number // 4), named(common, number - number // 4 - 1))
    mixed = jax.random.permutation(jax.random.fold_in(own, 3), amount)
    donor, receiver = mixed[0:amount // 2 * 2:2], mixed[1:amount // 2 * 2:2]
    room = jnp.minimum(sizes[donor] - 1, limit - sizes[receiver]) // 2
    room = jnp.where((donor == sequence[0]) | (receiver == sequence[0]) | (sizes[receiver] == 0), 0, jnp.maximum(room, 0))
    passed = jax.random.randint(jax.random.fold_in(own, 4), (amount // 2,), 0, 1 << 20) % (room + 1)
    sizes = sizes.at[donor].add(-passed).at[receiver].add(passed)
    labels = jnp.searchsorted(jnp.cumsum(sizes), jnp.arange(rows * top), side="right").astype(jnp.int32)
    grid = labels.reshape(top, rows).T
    grid = grid[jax.random.permutation(jax.random.fold_in(own, 1), rows)]
    turn = jax.random.randint(jax.random.fold_in(own, 2), (rows, 1), 0, top)
    return jnp.take_along_axis(grid, (jnp.arange(top)[None, :] + turn) % top, axis=1)


def load_shares(amount, total, reach, slope, full):
    weights = [(1 << 20) // math.isqrt(rank ** slope) + 1 for rank in range(1, amount + 1)]
    largest = reach if full else min(reach, max(-(-total // amount), total * weights[0] // sum(weights)))
    least = 1 if total - largest >= amount - 1 else 0
    counts, rest = [largest] + [least] * (amount - 1), total - largest - least * (amount - 1)
    while rest > 0:
        free = [i for i in range(1, amount) if counts[i] < largest] or [i for i in range(1, amount) if counts[i] < reach]
        pool, budget = sum([weights[i] for i in free]), rest
        for i in free:
            more = min(reach - counts[i], max(1, budget * weights[i] // pool), rest)
            counts[i] = counts[i] + more
            rest = rest - more
    return np.array(counts)


def scatter_about(rng, shape, width, bound, pieces=(), kind=jnp.bfloat16):
    level = steps_of(rng, shape, pieces, -0.22, 0.18) if pieces else 1.0
    values = jax.random.normal(rng, shape, jnp.float32) * width * level
    return jnp.minimum(jnp.maximum(values, -bound), bound).astype(kind)


def setup_inputs(seed: int = 0) -> dict:
    key_of = jax.random.split(jax.random.key(seed), 19)
    mixer_in = draw_mixer_in(jax.random.fold_in(key_of[18], 71), 0)
    mixer_gain = jnp.clip(1.0 + 0.18 * jax.random.normal(key_of[1], (D,), jnp.float32), 0.1, 1.9)
    query_weight = draw_query_weight(jax.random.fold_in(key_of[18], 71), 0)
    key_weight = draw_key_weight(jax.random.fold_in(key_of[18], 71), 0)
    value_weight = scatter_about(key_of[4], (D, HEADS * VDIM), D ** -0.5, 0.125, ((1, 4),))
    head_lambda = jnp.clip(0.3 + 0.5 * jax.random.uniform(key_of[5], (HEADS,), jnp.float32) ** steps_of(key_of[5], (HEADS,), ((0, 4),), -0.2, 0.2), 0.3, 0.8)
    head_gain = jnp.clip(1.0 + 0.18 * jax.random.normal(key_of[6], (VDIM,), jnp.float32), 0.1, 1.9)
    out_weight = scatter_about(key_of[7], (HEADS * VDIM, D), (HEADS * VDIM) ** -0.5, 0.25, ((0, 4),))
    expert_in = scatter_about(key_of[8], (TOKENS, D), 1.0, 6.0, ((0, 256),))
    expert_gain = jnp.clip(1.0 + 0.18 * jax.random.normal(key_of[9], (D,), jnp.float32), 0.1, 1.9)
    routes_keys = jax.random.split(jax.random.fold_in(key_of[10], 1), TOKENS // TOK_DEV)
    routes_turns = jax.random.permutation(jax.random.fold_in(key_of[10], 3), TOKENS // TOK_DEV)
    routes = jax.vmap(lambda own, number: assign_block(jax.random.fold_in(key_of[10], 2), own, number, TOK_DEV, EXPERTS, TOPK, CAP, 1))(routes_keys, routes_turns).reshape((TOKENS, TOPK))
    route_weights = jnp.clip(jnp.exp(math.log(1.0) - 2.3025851 * jax.random.uniform(key_of[11], (TOKENS, TOPK), jnp.float32) ** steps_of(key_of[11], (TOKENS, TOPK), ((0, 256),), -0.2, 0.2)), 0.1, 1.0)
    gate_weight = scatter_about(key_of[12], (EXPERTS, D, FE), D ** -0.5, 0.125, ((0, 64),))
    up_weight = scatter_about(key_of[13], (EXPERTS, D, FE), D ** -0.5, 0.125, ((0, 64),))
    down_weight = scatter_about(key_of[14], (EXPERTS, FE, D), FE ** -0.5, 0.25, ((0, 64),))
    shared_gate = scatter_about(key_of[15], (D, FS), D ** -0.5, 0.125, ((1, 4),))
    shared_up = scatter_about(key_of[16], (D, FS), D ** -0.5, 0.125, ((1, 4),))
    shared_down = scatter_about(key_of[17], (FS, D), FS ** -0.5, 0.25, ((0, 4),))
    return {"mixer_in": mixer_in, "mixer_gain": mixer_gain, "query_weight": query_weight, "key_weight": key_weight, "value_weight": value_weight, "head_lambda": head_lambda, "head_gain": head_gain, "out_weight": out_weight, "expert_in": expert_in, "expert_gain": expert_gain, "routes": routes, "route_weights": route_weights, "gate_weight": gate_weight, "up_weight": up_weight, "down_weight": down_weight, "shared_gate": shared_gate, "shared_up": shared_up, "shared_down": shared_down}


EPS = 1e-06
ROUTED_SCALE = 2.5

def rms_rows(matrix, scales):
    values_in = matrix.astype(jnp.float32)
    inverse = lax.rsqrt(lax.optimization_barrier(jnp.mean(values_in * values_in, axis=-1, keepdims=True)) + EPS)
    return values_in * inverse * scales

def attend_block(query_rows, key_head, value_head, lambda_head, head_gain):
    reads = []
    for map_index in range(2):
        lower = map_index * HALF
        scores = jnp.dot(query_rows[:, lower:lower + HALF], key_head[:, lower:lower + HALF].T, preferred_element_type=jnp.float32) * HALF ** (-0.5)
        row_top = lax.optimization_barrier(jnp.max(scores, axis=1, keepdims=True))
        exponent = jnp.exp(scores - row_top)
        row_total = lax.optimization_barrier(jnp.sum(exponent, axis=1, keepdims=True))
        weights = exponent.astype(jnp.bfloat16)
        reads.append(jnp.dot(weights, value_head, preferred_element_type=jnp.float32) / row_total)
    difference = reads[0] - lambda_head * reads[1]
    return (rms_rows(difference, head_gain) * (1.0 - lambda_head)).astype(jnp.bfloat16)

def mixer_half(mixer_in, mixer_gain, query_weight, key_weight, value_weight, head_lambda, head_gain, out_weight):
    normed = rms_rows(mixer_in, mixer_gain).astype(jnp.bfloat16)
    queries = jnp.dot(normed, query_weight, preferred_element_type=jnp.float32).astype(jnp.bfloat16)
    keys_all = jnp.dot(normed, key_weight, preferred_element_type=jnp.float32).astype(jnp.bfloat16)
    values_all = jnp.dot(normed, value_weight, preferred_element_type=jnp.float32).astype(jnp.bfloat16)
    length = normed.shape[0]
    block_rows = math.gcd(length, 512)
    head_outputs = []
    for head_index in range(HEADS):
        lower = head_index * 2 * HALF
        query_head = queries[:, lower:lower + 2 * HALF].reshape(length // block_rows, block_rows, 2 * HALF)
        key_head = keys_all[:, lower:lower + 2 * HALF]
        value_head = values_all[:, head_index * VDIM:(head_index + 1) * VDIM]
        worker = partial(attend_block, key_head=key_head, value_head=value_head, lambda_head=head_lambda[head_index], head_gain=head_gain)
        head_outputs.append(lax.map(worker, query_head).reshape(length, VDIM))
    attended = jnp.concatenate(head_outputs, axis=1)
    group_cols = HEADS // N_TP * VDIM
    mixed_sum = jnp.zeros((length, D), jnp.float32)
    for group_index in range(N_TP):
        lower = group_index * group_cols
        piece_out = jnp.dot(attended[:, lower:lower + group_cols], out_weight[lower:lower + group_cols], preferred_element_type=jnp.float32).astype(jnp.bfloat16)
        mixed_sum = mixed_sum + lax.optimization_barrier(piece_out).astype(jnp.float32)
    return mixed_sum.astype(jnp.bfloat16)

def expert_half(expert_in, expert_gain, routes, route_weights, gate_weight, up_weight, down_weight, shared_gate, shared_up, shared_down):
    normed = rms_rows(expert_in, expert_gain).astype(jnp.bfloat16)
    length = normed.shape[0]
    shares = ROUTED_SCALE * route_weights / lax.optimization_barrier(jnp.sum(route_weights, axis=1, keepdims=True))
    group_cols = FS // N_TP
    shared_sum = jnp.zeros((length, D), jnp.float32)
    for group_index in range(N_TP):
        lower = group_index * group_cols
        gate_part = jnp.dot(normed, shared_gate[:, lower:lower + group_cols], preferred_element_type=jnp.float32)
        up_part = jnp.dot(normed, shared_up[:, lower:lower + group_cols], preferred_element_type=jnp.float32)
        hidden = (jax.nn.silu(gate_part) * up_part).astype(jnp.bfloat16)
        piece_out = jnp.dot(hidden, shared_down[lower:lower + group_cols], preferred_element_type=jnp.float32).astype(jnp.bfloat16)
        shared_sum = shared_sum + lax.optimization_barrier(piece_out).astype(jnp.float32)
    device_count = length // TOK_DEV
    assigned = TOK_DEV * TOPK
    blocks = routes.reshape(device_count, assigned).astype(jnp.int32)
    onehot = (blocks[:, :, None] == jnp.arange(EXPERTS, dtype=jnp.int32)[None, None, :]).astype(jnp.int32)
    slot_rank = lax.optimization_barrier(jnp.sum((jnp.cumsum(onehot, axis=1) - onehot) * onehot, axis=2)).astype(jnp.int32)
    column = jnp.arange(device_count, dtype=jnp.int32)[:, None] * CAP + slot_rank
    assign_ids = jnp.arange(device_count * assigned, dtype=jnp.int32).reshape(device_count, assigned)
    table = jnp.full((EXPERTS, device_count * CAP), length * TOPK, jnp.int32).at[blocks, column].set(assign_ids)
    padded_rows = jnp.concatenate([normed, jnp.zeros((1, D), jnp.bfloat16)], axis=0)
    padded_shares = jnp.concatenate([shares.reshape(-1), jnp.zeros((1,), jnp.float32)], axis=0)

    def one_expert(running, inputs):
        assign_row, gate_one, up_one, down_one = inputs
        tokens = (assign_row // TOPK).astype(jnp.int32)
        token_rows = padded_rows[tokens]
        gate_part = jnp.dot(token_rows, gate_one, preferred_element_type=jnp.float32)
        up_part = jnp.dot(token_rows, up_one, preferred_element_type=jnp.float32)
        hidden = (jax.nn.silu(gate_part) * up_part).astype(jnp.bfloat16)
        result = jnp.dot(hidden, down_one, preferred_element_type=jnp.float32).astype(jnp.bfloat16)
        weighted = lax.optimization_barrier(result).astype(jnp.float32) * padded_shares[assign_row][:, None]
        return (running.at[tokens].add(weighted), None)
    start_sum = jnp.zeros((length + 1, D), jnp.float32)
    routed, unused = lax.scan(one_expert, start_sum, (table, gate_weight, up_weight, down_weight))
    return (routed[:length] + shared_sum).astype(jnp.bfloat16)

def reference(mixer_in, mixer_gain, query_weight, key_weight, value_weight, head_lambda, head_gain, out_weight, expert_in, expert_gain, routes, route_weights, gate_weight, up_weight, down_weight, shared_gate, shared_up, shared_down):
    mixed_out = mixer_half(mixer_in, mixer_gain, query_weight, key_weight, value_weight, head_lambda, head_gain, out_weight)
    expert_out = expert_half(expert_in, expert_gain, routes, route_weights, gate_weight, up_weight, down_weight, shared_gate, shared_up, shared_down)
    return (mixed_out, expert_out)
```

```python
import functools
import math

import jax
import jax.numpy as jnp
from jax import lax
from jax.experimental import pallas as pl
from jax.experimental.pallas import tpu as pltpu
from jax.sharding import Mesh
from jax.sharding import PartitionSpec as P

EP = ("ep_0", "ep_1", "ep_2")
EP_TP = ("ep_0", "ep_1", "ep_2", "tp")
EPS = 1e-06
ROUTED_SCALE = 2.5
LOG2E = 1.4426950408889634
BF = jnp.bfloat16
F32 = jnp.float32
VMEM = pl.BlockSpec(memory_space=pltpu.VMEM)
SMEM = pl.BlockSpec(memory_space=pltpu.SMEM)


def shift(x, axis, k):
    n = lax.axis_size(axis)
    return lax.ppermute(x, axis, [(i, (i + k) % n) for i in range(n)])


def call(kernel, name, ins, out_shape, flops, nbytes, trans=0, vmem=24, scratch=(), smem_out=()):
    single = not isinstance(out_shape, (list, tuple))
    outs = [out_shape] if single else list(out_shape)
    specs = [SMEM if i in smem_out else VMEM for i in range(len(outs))]
    return pl.pallas_call(
        kernel,
        name=name,
        out_shape=outs[0] if single else outs,
        in_specs=[spec for _, spec in ins],
        out_specs=specs[0] if single else specs,
        scratch_shapes=list(scratch),
        compiler_params=pltpu.CompilerParams(vmem_limit_bytes=vmem * 2**20),
        cost_estimate=pl.CostEstimate(flops=flops, bytes_accessed=nbytes, transcendentals=trans),
    )(*[a for a, _ in ins])


def ring4(x, axis):
    fwd = shift(x, axis, 1)
    bwd = shift(x, axis, -1)
    half = x.shape[0] // 2
    return x, fwd, bwd, shift(fwd[:half], axis, 1), shift(bwd[half:], axis, -1)


def rms_rows(matrix, scales):
    values_in = matrix.astype(F32)
    inverse = lax.rsqrt(jnp.mean(values_in * values_in, axis=-1, keepdims=True) + EPS)
    return values_in * inverse * scales


def project_kernel(r0, r1, r2, r3, r4, wq, wk, wv, q_ref, kv_ref):
    rows = jnp.concatenate([r0[...], r1[...], r2[...], r3[...], r4[...]], axis=0)
    width = wq.shape[1]
    q_ref[...] = jnp.dot(rows, wq[...], preferred_element_type=F32).astype(BF)
    kv_ref[:, :width] = jnp.dot(rows, wk[...], preferred_element_type=F32).astype(BF)
    kv_ref[:, width:] = jnp.dot(rows, wv[...], preferred_element_type=F32).astype(BF)


def shared_kernel(r0, r1, r2, r3, r4, wg, wu, h0, h1, h2, h3):
    rows = jnp.concatenate([r0[...], r1[...], r2[...], r3[...], r4[...]], axis=0)
    gate = jnp.dot(rows, wg[...], preferred_element_type=F32)
    up = jnp.dot(rows, wu[...], preferred_element_type=F32)
    hidden = (gate / (1.0 + jnp.exp(-gate)) * up).astype(BF)
    n = r0.shape[0]
    for i, h in enumerate((h0, h1, h2, h3)):
        h[...] = hidden[i * n : (i + 1) * n]


def split3(x):
    hi = x.astype(BF)
    rest = x - hi.astype(F32)
    mid = rest.astype(BF)
    low = (rest - mid.astype(F32)).astype(BF)
    return hi, mid, low


def store_lse(ref, index, rows, lse):
    hi, mid, low = split3(lse)
    packed = jnp.concatenate(
        [hi.astype(F32), mid.astype(F32), low.astype(F32), jnp.zeros_like(lse)], axis=0
    ).astype(BF)
    if index is None:
        ref[rows:, :] = packed
    else:
        ref[index, rows:, :] = packed


def load_lse(block):
    b = block.astype(F32)
    return b[0:8] + b[8:16] + b[16:24]


def attend_kernel(half, q0, q1, q2, q3, *refs):
    kvs, (own, peer), (k_ref, v_ref, q_all) = refs[:9], refs[9:11], refs[11:]
    width = k_ref.shape[1]
    at = 0
    for kv in kvs:
        n = kv.shape[0]
        k_ref[at : at + n, :] = kv[:, :width]
        v_ref[at : at + n, :] = kv[:, width:]
        at += n
    nq = q0.shape[0] // 2
    groups = nq // 128
    lane = lax.broadcasted_iota(jnp.int32, (1, width), 1)
    eye = lax.broadcasted_iota(jnp.int32, (128, 128), 0) == lax.broadcasted_iota(
        jnp.int32, (128, 128), 1
    )
    scale = half ** (-0.5)
    for y, q_ref in enumerate((q0, q1, q2, q3)):
        q_all[y] = q_ref[...]
    for core, out in enumerate((own, peer)):

        @pl.loop(0, 4)
        def _(y, core=core, out=out):
            q = q_all[y, core * nq : (core + 1) * nq, :]
            rows = []
            for c in range(2):
                qm = jnp.where((lane // half) == c, q, jnp.zeros_like(q))
                s = lax.dot_general(
                    qm, k_ref[...], (((1,), (1,)), ((), ())), preferred_element_type=F32
                )
                top = jnp.max(s, axis=1, keepdims=True)
                p = jnp.exp2((s - top) * (LOG2E * scale))
                total = jnp.sum(p, axis=1, keepdims=True)
                o = jnp.dot(p.astype(BF), v_ref[...], preferred_element_type=F32)
                out[y, c * nq : (c + 1) * nq, :] = (o / total).astype(BF)
                lse = top * scale + jnp.log(total)
                for g in range(groups):
                    col = lse[g * 128 : (g + 1) * 128]
                    rows.append(jnp.sum(jnp.where(eye, col, 0.0), axis=0, keepdims=True))
            rows += [jnp.zeros((1, 128), F32)] * (8 - len(rows))
            store_lse(out, y, 2 * nq, jnp.concatenate(rows, axis=0))


def row_weights(w, g):
    return jnp.transpose(jnp.broadcast_to(w[g : g + 1, :], (128, 128)))


def merge_cores_kernel(own, rec, o0, o1, o2, o3):
    nrow = own.shape[1] - 32
    for y, out in enumerate((o0, o1, o2, o3)):
        la = load_lse(own[y, nrow:, :])
        lb = load_lse(rec[y, nrow:, :])
        top = jnp.maximum(la, lb)
        wa = jnp.exp(la - top)
        wb = jnp.exp(lb - top)
        total = wa + wb
        fa = wa / total
        fb = wb / total
        for g in range(nrow // 128):
            sl = slice(g * 128, (g + 1) * 128)
            out[sl, :] = (
                row_weights(fa, g) * own[y, sl, :].astype(F32)
                + row_weights(fb, g) * rec[y, sl, :].astype(F32)
            ).astype(BF)
        store_lse(out, None, nrow, top + jnp.log(total))


def merge_all_kernel(lam, p0, p1, p2, p3, gain, a0, a1, a2, a3, att):
    parts = (p0, p1, p2, p3)
    nrow = p0.shape[0] - 32
    lses = [load_lse(p[nrow:, :]) for p in parts]
    top = functools.reduce(jnp.maximum, lses)
    ws = [jnp.exp(x - top) for x in lses]
    total = functools.reduce(jnp.add, ws)
    fs = [w / total for w in ws]
    nq = nrow // 2
    lam0 = lam[0]
    for g in range(nq // 128):
        reads = []
        for c in range(2):
            at = c * nq + g * 128
            idx = at // 128
            acc = 0.0
            for f, p in zip(fs, parts):
                acc = acc + row_weights(f, idx) * p[at : at + 128, :].astype(F32)
            reads.append(acc)
        diff = reads[0] - lam0 * reads[1]
        inv = lax.rsqrt(jnp.mean(diff * diff, axis=1, keepdims=True) + EPS)
        att[g * 128 : (g + 1) * 128, :] = (diff * inv * gain[...] * (1.0 - lam0)).astype(BF)
    n = a0.shape[0]
    for i, a in enumerate((a0, a1, a2, a3)):
        a[...] = att[i * n : (i + 1) * n, :]


def project_out_kernel(offset, extra, *refs):
    pieces, weights = refs[:4], refs[4:9]
    out = refs[-1]
    w0, wf, wb, wh0, wh1 = weights
    n = w0.shape[0] // 2
    half = n // 2
    lo, hi = offset * n, (offset + 1) * n
    far = wh0 if offset == 0 else wh1
    total = None
    for a, w in zip(pieces, (w0[lo:hi, :], wb[lo:hi, :], wf[lo:hi, :], far[...])):
        part = jnp.dot(a[...], w, preferred_element_type=F32).astype(BF).astype(F32)
        total = part if total is None else total + part
    if extra:
        total = total + refs[9][...]
    out[...] = total.astype(out.dtype)


def dispatch_kernel(capacity, top_count, x_ref, gain, routes, out, slots, xf, count):
    x = x_ref[...].astype(F32)
    tokens = x.shape[0]
    width = x.shape[1] * x.shape[2]
    ms = jnp.sum(x * x, axis=(1, 2), keepdims=True) * (1.0 / width)
    xf[...] = (x * lax.rsqrt(ms + EPS) * gain[...]).astype(BF)
    out[...] = jnp.zeros_like(out)
    for e in range(count.shape[0]):
        count[e] = 0

    def step(t, carry):
        row = xf[t]
        for k in range(top_count):
            i = t * top_count + k
            e = routes[i]
            c = count[e]
            count[e] = c + 1
            s = e * capacity + c
            slots[i] = s
            out[s] = row
        return carry

    lax.fori_loop(0, tokens, step, 0)


def combine_kernel(top_count, ret, slots, shares, out):
    def step(t, carry):
        acc = None
        for k in range(top_count):
            i = t * top_count + k
            v = ret[slots[i]].astype(F32) * shares[i]
            acc = v if acc is None else acc + v
        out[t] = acc
        return carry

    lax.fori_loop(0, out.shape[0], step, 0)


def on_device(
    mixer_in,
    mixer_gain,
    query_weight,
    key_weight,
    value_weight,
    head_lambda,
    head_gain,
    out_weight,
    expert_in,
    expert_gain,
    routes,
    route_weights,
    gate_weight,
    up_weight,
    down_weight,
    shared_gate,
    shared_up,
    shared_down,
):
    tokens, width = mixer_in.shape
    vdim = head_gain.shape[0]
    half = query_weight.shape[1] // 2
    nq = 4 * tokens
    experts = lax.axis_size(EP)
    top_count = routes.shape[1]
    capacity = 2 * tokens * top_count // experts
    slots_all = experts * capacity
    lanes = 128
    subs = width // lanes
    S = jax.ShapeDtypeStruct

    flat_routes = routes.reshape(-1)
    shares = ROUTED_SCALE * route_weights / jnp.sum(route_weights, axis=1, keepdims=True)
    outgoing, slot_index = call(
        functools.partial(dispatch_kernel, capacity, top_count),
        "dispatch",
        [
            (expert_in.reshape(tokens, subs, lanes), VMEM),
            (expert_gain.reshape(1, subs, lanes), VMEM),
            (flat_routes, SMEM),
        ],
        [S((slots_all, subs, lanes), BF), S((tokens * top_count,), jnp.int32)],
        flops=10**7,
        nbytes=2 * 10**6,
        scratch=[pltpu.VMEM((tokens, subs, lanes), BF), pltpu.SMEM((experts,), jnp.int32)],
        smem_out=(1,),
    )
    arrived = lax.all_to_all(
        outgoing.reshape(experts, capacity * subs, lanes), EP, 0, 0, tiled=True
    )

    normed_mixer = rms_rows(mixer_in, mixer_gain).astype(BF)
    mixer_rows = ring4(normed_mixer, "tp")
    queries, kv = call(
        project_kernel,
        "project",
        [(r, VMEM) for r in mixer_rows]
        + [(query_weight, VMEM), (key_weight, VMEM), (value_weight, VMEM)],
        [S((nq, 2 * half), BF), S((nq, 2 * half + vdim), BF)],
        flops=2 * nq * width * (4 * half + vdim),
        nbytes=4 * 10**6,
    )
    kvs = [kv]
    fwd = bwd = kv
    for _ in range(3):
        fwd, bwd = shift(fwd, "ep_0", 1), shift(bwd, "ep_0", -1)
        kvs += [fwd, bwd]
    kvs += [shift(fwd[: nq // 2], "ep_0", 1), shift(bwd[nq // 2 :], "ep_0", -1)]
    q_pair = jnp.concatenate([queries, shift(queries, "ep_2", 1)], axis=0)
    q_all = [q_pair] + [shift(q_pair, "ep_1", k) for k in (1, -1, 2)]

    normed_expert = rms_rows(expert_in, expert_gain).astype(BF)
    normed_expert, _ = lax.optimization_barrier((normed_expert, mixer_rows[3]))
    expert_rows = ring4(normed_expert, "tp")
    tail_weights = jnp.concatenate([out_weight, shared_down], axis=0)
    tail_weights, _ = lax.optimization_barrier((tail_weights, expert_rows[3]))
    tails = ring4(tail_weights, "tp")
    hidden = call(
        shared_kernel,
        "shared",
        [(r, VMEM) for r in expert_rows] + [(shared_gate, VMEM), (shared_up, VMEM)],
        [S((tokens, vdim), BF)] * 4,
        flops=4 * nq * width * vdim,
        nbytes=3 * 10**6,
    )
    hidden = [hidden[0]] + [shift(h, "tp", k) for h, k in zip(hidden[1:], (-1, 1, 2))]
    shared_sum = call(
        functools.partial(project_out_kernel, 1, False),
        "shared_out",
        [(a, VMEM) for a in hidden] + [(w, VMEM) for w in tails],
        S((tokens, width), F32),
        flops=8 * tokens * vdim * width,
        nbytes=5 * 10**6,
    )

    token_rows = arrived.reshape(slots_all, width)
    gate_part = jnp.dot(token_rows, gate_weight[0], preferred_element_type=F32)
    up_part = jnp.dot(token_rows, up_weight[0], preferred_element_type=F32)
    expert_hidden = (jax.nn.silu(gate_part) * up_part).astype(BF)
    result = jnp.dot(expert_hidden, down_weight[0], preferred_element_type=F32).astype(BF)
    returned = lax.all_to_all(
        result.reshape(experts, capacity * subs, lanes), EP, 0, 0, tiled=True
    )

    message = S((4, 2 * nq + 32, vdim), BF)
    keys = 8 * nq
    own, peer = call(
        functools.partial(attend_kernel, half),
        "attend",
        [(q, VMEM) for q in q_all] + [(b, VMEM) for b in kvs],
        [message, message],
        flops=2 * 2 * 8 * nq * keys * (2 * half + vdim),
        nbytes=6 * 10**6,
        trans=2 * 8 * nq * keys,
        vmem=48,
        scratch=[
            pltpu.VMEM((keys, 2 * half), BF),
            pltpu.VMEM((keys, vdim), BF),
            pltpu.VMEM((4, 2 * nq, 2 * half), BF),
        ],
    )
    merged = call(
        merge_cores_kernel,
        "merge_cores",
        [(own, VMEM), (shift(peer, "ep_2", 1), VMEM)],
        [S((2 * nq + 32, vdim), BF)] * 4,
        flops=5 * 10**7,
        nbytes=3 * 10**6,
    )
    parts = [merged[0]] + [shift(m, "ep_1", k) for m, k in zip(merged[1:], (-1, 1, 2))]
    attended = call(
        merge_all_kernel,
        "merge_all",
        [(head_lambda, SMEM)] + [(p, VMEM) for p in parts] + [(head_gain.reshape(1, vdim), VMEM)],
        [S((tokens, vdim), BF)] * 4,
        flops=5 * 10**7,
        nbytes=10**6,
        scratch=[pltpu.VMEM((nq, vdim), BF)],
    )
    attended = [attended[0]] + [shift(a, "tp", k) for a, k in zip(attended[1:], (-1, 1, 2))]
    mixed_out = call(
        functools.partial(project_out_kernel, 0, False),
        "mixed_out",
        [(a, VMEM) for a in attended] + [(w, VMEM) for w in tails],
        S((tokens, width), BF),
        flops=8 * tokens * vdim * width,
        nbytes=5 * 10**6,
    )

    routed = call(
        functools.partial(combine_kernel, top_count),
        "combine",
        [
            (returned.reshape(slots_all, subs, lanes), VMEM),
            (slot_index, SMEM),
            (shares.reshape(-1), SMEM),
        ],
        S((tokens, subs, lanes), F32),
        flops=10**7,
        nbytes=3 * 10**6,
    )
    expert_out = (routed.reshape(tokens, width) + shared_sum).astype(BF)
    return (mixed_out, expert_out)


def solution(mesh):
    split = Mesh(mesh.devices.reshape(8, 4, 2, mesh.shape["tp"]), ("ep_0", "ep_1", "ep_2", "tp"))
    placed = (
        P(EP_TP, None),
        P(),
        P(None, "tp"),
        P(None, "tp"),
        P(None, "tp"),
        P("tp"),
        P(),
        P("tp", None),
        P(EP_TP, None),
        P(),
        P(EP_TP, None),
        P(EP_TP, None),
        P(EP, None, None),
        P(EP, None, None),
        P(EP, None, None),
        P(None, "tp"),
        P(None, "tp"),
        P("tp", None),
    )
    return jax.shard_map(
        on_device,
        mesh=split,
        in_specs=placed,
        out_specs=(P(EP_TP, None), P(EP_TP, None)),
        check_vma=False,
    )
```

```python
import functools

import jax
import jax.numpy as jnp
from jax import lax
from jax.experimental import pallas as pl
from jax.experimental.pallas import tpu as pltpu
from jax.sharding import Mesh
from jax.sharding import PartitionSpec as P


EP = ("ep_0", "ep_1", "ep_2")
EP_TP = ("ep_0", "ep_1", "ep_2", "tp")
EPS = 1e-06
ROUTED_SCALE = 2.5
LOG2E = 1.4426950408889634
BF = jnp.bfloat16
F32 = jnp.float32
VMEM = pl.BlockSpec(memory_space=pltpu.VMEM)
SMEM = pl.BlockSpec(memory_space=pltpu.SMEM)


def shift(x, axis, k):
    n = lax.axis_size(axis)
    return lax.ppermute(x, axis, [(i, (i + k) % n) for i in range(n)])


def call(kernel, ins, out_shape, flops, nbytes, trans=0, vmem=24, scratch=(), smem_out=()):
    single = not isinstance(out_shape, (list, tuple))
    outs = [out_shape] if single else list(out_shape)
    specs = [SMEM if i in smem_out else VMEM for i in range(len(outs))]
    return pl.pallas_call(
        kernel,
        out_shape=outs[0] if single else outs,
        in_specs=[spec for _, spec in ins],
        out_specs=specs[0] if single else specs,
        scratch_shapes=list(scratch),
        compiler_params=pltpu.CompilerParams(vmem_limit_bytes=vmem * 2**20),
        cost_estimate=pl.CostEstimate(flops=flops, bytes_accessed=nbytes, transcendentals=trans),
    )(*[a for a, _ in ins])


def ring4(x, axis, far):
    fwd = shift(x, axis, 1)
    bwd = shift(x, axis, -1)
    return x, fwd, bwd, shift(fwd if far > 0 else bwd, axis, far)


def rms_rows(matrix, scales):
    values_in = matrix.astype(F32)
    inverse = lax.rsqrt(jnp.mean(values_in * values_in, axis=-1, keepdims=True) + EPS)
    return values_in * inverse * scales


def project_kernel(r0, r1, r2, r3, wq, wk, wv, q_ref, kv_ref):
    rows = jnp.concatenate([r0[...], r1[...], r2[...], r3[...]], axis=0)
    width = wq.shape[1]
    q_ref[...] = jnp.dot(rows, wq[...], preferred_element_type=F32).astype(BF)
    kv_ref[:, :width] = jnp.dot(rows, wk[...], preferred_element_type=F32).astype(BF)
    kv_ref[:, width:] = jnp.dot(rows, wv[...], preferred_element_type=F32).astype(BF)


def silu_product(gate, up):
    return (gate / (1.0 + jnp.exp(-gate)) * up).astype(BF)


def shared_kernel(n, x0, x1, x2, x3, wg, wu, h0, h1, h2, h3):
    rows = jnp.concatenate([x[:n, :] for x in (x0, x1, x2, x3)], axis=0)
    gate = jnp.dot(rows, wg[...], preferred_element_type=F32)
    up = jnp.dot(rows, wu[...], preferred_element_type=F32)
    hidden = silu_product(gate, up)
    for i, h in enumerate((h0, h1, h2, h3)):
        h[...] = hidden[i * n : (i + 1) * n]


def to_tiles(tiles, rows):
    count, subs = rows.shape[0], rows.shape[1] // 128
    for j in range(subs):
        tiles[pl.ds(j, count, stride=subs), :] = rows[:, j * 128 : (j + 1) * 128]


def from_tiles(tiles, out):
    count, subs = out.shape[0], out.shape[1] // 128
    for j in range(subs):
        block = tiles[pl.ds(j, count, stride=subs), :]
        out[:, j * 128 : (j + 1) * 128] = block.astype(out.dtype)


def expert_kernel(x_ref, wg, wu, wd, out, tiles, rows):
    shape = x_ref.shape
    tiles[...] = x_ref[...].reshape(tiles.shape).astype(F32)
    from_tiles(tiles, rows)
    x = rows[...]
    gate = jnp.dot(x, wg[0], preferred_element_type=F32)
    up = jnp.dot(x, wu[0], preferred_element_type=F32)
    hidden = silu_product(gate, up)
    to_tiles(tiles, jnp.dot(hidden, wd[0], preferred_element_type=F32))
    out[...] = tiles[...].astype(BF).reshape(shape)


def split3(x):
    hi = x.astype(BF)
    rest = x - hi.astype(F32)
    mid = rest.astype(BF)
    low = (rest - mid.astype(F32)).astype(BF)
    return hi, mid, low


def store_lse(ref, index, rows, lse):
    hi, mid, low = split3(lse)
    packed = jnp.concatenate(
        [hi.astype(F32), mid.astype(F32), low.astype(F32), jnp.zeros_like(lse)], axis=0
    ).astype(BF)
    if index is None:
        ref[rows:, :] = packed
    else:
        ref[index, rows:, :] = packed


def load_lse(block):
    b = block.astype(F32)
    return b[0:8] + b[8:16] + b[16:24]


def attend_kernel(half, q0, q1, q2, q3, *refs):
    kvs, (own, peer), (k_ref, v_ref, q_all, o_all, s_ref, top_ref) = refs[:8], refs[8:10], refs[10:]
    width = k_ref.shape[1]
    at = 0
    for kv in kvs:
        n = kv.shape[0]
        k_ref[at : at + n, :] = kv[:, :width]
        v_ref[at : at + n, :] = kv[:, width:]
        at += n
    nq = q0.shape[0] // 2
    groups = nq // 128
    lane = lax.broadcasted_iota(jnp.int32, (1, width), 1)
    eye = lax.broadcasted_iota(jnp.int32, (128, 128), 0) == lax.broadcasted_iota(
        jnp.int32, (128, 128), 1
    )
    scale = half ** (-0.5)
    for y, q_ref in enumerate((q0, q1, q2, q3)):
        q_all[y] = q_ref[:nq, :]
        q_all[4 + y] = q_ref[nq:, :]

    def scores(y, c):
        q = q_all[y]
        qm = jnp.where((lane // half) == c, q, jnp.zeros_like(q))
        s = lax.dot_general(qm, k_ref[...], (((1,), (1,)), ((), ())), preferred_element_type=F32)
        s_ref[c] = s
        top_ref[c] = jnp.max(s, axis=1, keepdims=True)

    def read(y, c):
        top = top_ref[c]
        p = jnp.exp2((s_ref[c] - top) * (LOG2E * scale))
        total = jnp.sum(p, axis=1, keepdims=True)
        o = jnp.dot(p.astype(BF), v_ref[...], preferred_element_type=F32)
        o_all[y, c * nq : (c + 1) * nq, :] = (o / total).astype(BF)
        lse = top * scale + jnp.log(total)
        return [
            jnp.sum(jnp.where(eye, lse[g * 128 : (g + 1) * 128], 0.0), axis=0, keepdims=True)
            for g in range(groups)
        ]

    scores(0, 0)

    @pl.loop(0, 8)
    def _(y):
        scores(y, 1)
        rows = read(y, 0)
        scores(jnp.minimum(y + 1, 7), 0)
        rows += read(y, 1)
        rows += [jnp.zeros((1, 128), F32)] * (8 - len(rows))
        store_lse(o_all, y, 2 * nq, jnp.concatenate(rows, axis=0))

    own[...] = o_all[:4]
    peer[...] = o_all[4:]


def row_weights(w, g):
    return jnp.transpose(jnp.broadcast_to(w[g : g + 1, :], (128, 128)))


def merge_cores_kernel(own, rec, o0, o1, o2, o3):
    nrow = own.shape[1] - 32
    for y, out in enumerate((o0, o1, o2, o3)):
        la = load_lse(own[y, nrow:, :])
        lb = load_lse(rec[y, nrow:, :])
        top = jnp.maximum(la, lb)
        wa = jnp.exp(la - top)
        wb = jnp.exp(lb - top)
        total = wa + wb
        fa = wa / total
        fb = wb / total
        for g in range(nrow // 128):
            sl = slice(g * 128, (g + 1) * 128)
            out[sl, :] = (
                row_weights(fa, g) * own[y, sl, :].astype(F32)
                + row_weights(fb, g) * rec[y, sl, :].astype(F32)
            ).astype(BF)
        store_lse(out, None, nrow, top + jnp.log(total))


def merge_all_kernel(lam, p0, p1, p2, p3, gain, h0, h1, h2, h3, a0, a1, a2, a3, att):
    parts = (p0, p1, p2, p3)
    nrow = p0.shape[0] - 32
    lses = [load_lse(p[nrow:, :]) for p in parts]
    top = functools.reduce(jnp.maximum, lses)
    ws = [jnp.exp(x - top) for x in lses]
    total = functools.reduce(jnp.add, ws)
    fs = [w / total for w in ws]
    nq = nrow // 2
    lam0 = lam[0]
    for g in range(nq // 128):
        reads = []
        for c in range(2):
            at = c * nq + g * 128
            idx = at // 128
            acc = 0.0
            for f, p in zip(fs, parts):
                acc = acc + row_weights(f, idx) * p[at : at + 128, :].astype(F32)
            reads.append(acc)
        diff = reads[0] - lam0 * reads[1]
        inv = lax.rsqrt(jnp.mean(diff * diff, axis=1, keepdims=True) + EPS)
        att[g * 128 : (g + 1) * 128, :] = (diff * inv * gain[...] * (1.0 - lam0)).astype(BF)
    n = h0.shape[0]
    for i, (a, h) in enumerate(((a0, h0), (a1, h1), (a2, h2), (a3, h3))):
        a[:n, :] = att[i * n : (i + 1) * n, :]
        a[n:, :] = h[...]


def project_out_kernel(n, a0, a1, a2, a3, wo, wd, x1, x2, x3, routed, mixed, expert):
    depth = wo.shape[0]
    for i, (own, extra, out) in enumerate(((wo, None, mixed), (wd, routed, expert))):
        lo, hi = n + i * depth, n + (i + 1) * depth
        total = None if extra is None else extra[...]
        for a, w in zip((a0, a1, a2, a3), (own, x2, x1, x3)):
            rows = w[...] if w is own else w[lo:hi, :]
            part = jnp.dot(a[i * n : (i + 1) * n, :], rows, preferred_element_type=F32)
            part = part.astype(BF).astype(F32)
            total = part if total is None else total + part
        out[...] = total.astype(out.dtype)


def dispatch_kernel(capacity, top_count, x_ref, gain, routes, out, normed, slots, tiles, xf, count):
    x = x_ref[...].astype(F32)
    inverse = lax.rsqrt(jnp.mean(x * x, axis=1, keepdims=True) + EPS)
    x = x * inverse * gain[...]
    normed[...] = x.astype(BF)
    to_tiles(tiles, x)
    xf[...] = tiles[...].astype(BF).reshape(xf.shape)
    out[...] = jnp.zeros_like(out)
    for e in range(count.shape[0]):
        count[e] = 0

    def step(t, carry):
        row = xf[t]
        for k in range(top_count):
            i = t * top_count + k
            e = routes[i]
            c = count[e]
            count[e] = c + 1
            s = e * capacity + c
            slots[i] = s
            out[s] = row
        return carry

    lax.fori_loop(0, x_ref.shape[0], step, 0)


def combine_kernel(top_count, ret, slots, shares, out, tiles):
    subs = ret.shape[1]

    def step(t, carry):
        acc = None
        for k in range(top_count):
            i = t * top_count + k
            v = ret[slots[i]].astype(F32) * shares[i]
            acc = v if acc is None else acc + v
        tiles[pl.ds(pl.multiple_of(t * subs, subs), subs), :] = acc
        return carry

    lax.fori_loop(0, out.shape[0], step, 0)
    from_tiles(tiles, out)


def on_device(
    mixer_in,
    mixer_gain,
    query_weight,
    key_weight,
    value_weight,
    head_lambda,
    head_gain,
    out_weight,
    expert_in,
    expert_gain,
    routes,
    route_weights,
    gate_weight,
    up_weight,
    down_weight,
    shared_gate,
    shared_up,
    shared_down,
):
    tokens, width = mixer_in.shape
    vdim = head_gain.shape[0]
    half = query_weight.shape[1] // 2
    nq = 4 * tokens
    experts = lax.axis_size(EP)
    top_count = routes.shape[1]
    capacity = 2 * tokens * top_count // experts
    slots_all = experts * capacity
    lanes = 128
    subs = width // lanes
    S = jax.ShapeDtypeStruct

    normed_mixer = rms_rows(mixer_in, mixer_gain).astype(BF)
    shares = ROUTED_SCALE * route_weights / jnp.sum(route_weights, axis=1, keepdims=True)
    normed_mixer, shares = lax.optimization_barrier((normed_mixer, shares.reshape(-1)))
    mixer_rows = ring4(normed_mixer, "tp", 1)
    queries, kv = call(
        project_kernel,
        [(r, VMEM) for r in mixer_rows]
        + [(query_weight, VMEM), (key_weight, VMEM), (value_weight, VMEM)],
        [S((nq, 2 * half), BF), S((nq, 2 * half + vdim), BF)],
        flops=2 * nq * width * (4 * half + vdim),
        nbytes=4 * 10**6,
        vmem=12,
    )

    flat_routes = routes.reshape(-1)
    outgoing, normed_expert, slot_index = call(
        functools.partial(dispatch_kernel, capacity, top_count),
        [
            (expert_in, VMEM),
            (expert_gain.reshape(1, width), VMEM),
            (flat_routes, SMEM),
        ],
        [
            S((slots_all, subs, lanes), BF),
            S((tokens, width), BF),
            S((tokens * top_count,), jnp.int32),
        ],
        flops=10**7,
        nbytes=2 * 10**6,
        scratch=[
            pltpu.VMEM((tokens * subs, lanes), F32),
            pltpu.VMEM((tokens, subs, lanes), BF),
            pltpu.SMEM((experts,), jnp.int32),
        ],
        smem_out=(2,),
        vmem=12,
    )
    arrived = lax.all_to_all(
        outgoing.reshape(experts, capacity * subs, lanes), EP, 0, 0, tiled=True
    )

    kvs = [kv]
    fwd = bwd = kv
    for _ in range(3):
        fwd = shift(fwd, "ep_0", 1)
        bwd = shift(bwd, "ep_0", -1)
        kvs += [fwd, bwd]
    kvs += [shift(fwd, "ep_0", 1)]
    q_pair = jnp.concatenate([queries, shift(queries, "ep_2", 1)], axis=0)
    q_all = [q_pair] + [shift(q_pair, "ep_1", k) for k in (1, -1, 2)]

    normed_expert, _ = lax.optimization_barrier((normed_expert, mixer_rows[3]))
    joined = jnp.concatenate([normed_expert, out_weight, shared_down], axis=0)
    tails = ring4(joined, "tp", -1)
    hidden = call(
        functools.partial(shared_kernel, tokens),
        [(r, VMEM) for r in tails] + [(shared_gate, VMEM), (shared_up, VMEM)],
        [S((tokens, vdim), BF)] * 4,
        flops=4 * nq * width * vdim,
        nbytes=3 * 10**6,
        vmem=12,
    )

    result = call(
        expert_kernel,
        [
            (arrived.reshape(slots_all, subs, lanes), VMEM),
            (gate_weight, VMEM),
            (up_weight, VMEM),
            (down_weight, VMEM),
        ],
        S((slots_all, subs, lanes), BF),
        flops=6 * slots_all * width * gate_weight.shape[2],
        nbytes=10 * 10**6,
        scratch=[pltpu.VMEM((slots_all * subs, lanes), F32), pltpu.VMEM((slots_all, width), BF)],
        vmem=20,
    )
    returned = lax.all_to_all(result.reshape(experts, capacity * subs, lanes), EP, 0, 0, tiled=True)

    message = S((4, 2 * nq + 32, vdim), BF)
    keys = 8 * nq
    own, peer = call(
        functools.partial(attend_kernel, half),
        [(q, VMEM) for q in q_all] + [(b, VMEM) for b in kvs],
        [message, message],
        flops=2 * 2 * 8 * nq * keys * (2 * half + vdim),
        nbytes=6 * 10**6,
        trans=2 * 8 * nq * keys,
        vmem=32,
        scratch=[
            pltpu.VMEM((keys, 2 * half), BF),
            pltpu.VMEM((keys, vdim), BF),
            pltpu.VMEM((8, nq, 2 * half), BF),
            pltpu.VMEM((8, 2 * nq + 32, vdim), BF),
            pltpu.VMEM((2, nq, keys), F32),
            pltpu.VMEM((2, nq, 1), F32),
        ],
    )
    merged = call(
        merge_cores_kernel,
        [(own, VMEM), (shift(peer, "ep_2", 1), VMEM)],
        [S((2 * nq + 32, vdim), BF)] * 4,
        flops=5 * 10**7,
        nbytes=3 * 10**6,
        vmem=8,
    )
    parts = [merged[0]]
    for i, k in enumerate((-1, 1, 2)):
        parts.append(shift(merged[i + 1], "ep_1", k))
    attended = call(
        merge_all_kernel,
        [(head_lambda, SMEM)]
        + [(p, VMEM) for p in parts]
        + [(head_gain.reshape(1, vdim), VMEM)]
        + [(h, VMEM) for h in hidden],
        [S((2 * tokens, vdim), BF)] * 4,
        flops=5 * 10**7,
        nbytes=10**6,
        scratch=[pltpu.VMEM((nq, vdim), BF)],
        vmem=8,
    )
    backs = [attended[0]]
    for i, k in enumerate((-1, 1, 2)):
        backs.append(shift(attended[i + 1], "tp", k))
    routed = call(
        functools.partial(combine_kernel, top_count),
        [
            (returned.reshape(slots_all, subs, lanes), VMEM),
            (slot_index, SMEM),
            (shares, SMEM),
        ],
        S((tokens, width), F32),
        flops=10**7,
        nbytes=3 * 10**6,
        scratch=[pltpu.VMEM((tokens * subs, lanes), F32)],
        vmem=8,
    )
    mixed_out, expert_out = call(
        functools.partial(project_out_kernel, tokens),
        [(a, VMEM) for a in backs]
        + [(out_weight, VMEM), (shared_down, VMEM)]
        + [(w, VMEM) for w in tails[1:]]
        + [(routed, VMEM)],
        [S((tokens, width), BF), S((tokens, width), BF)],
        flops=16 * tokens * vdim * width,
        nbytes=8 * 10**6,
        vmem=12,
    )

    return (mixed_out, expert_out)


def solution(mesh):
    split = Mesh(mesh.devices.reshape(8, 4, 2, mesh.shape["tp"]), ("ep_0", "ep_1", "ep_2", "tp"))
    placed = (
        P(EP_TP, None),
        P(),
        P(None, "tp"),
        P(None, "tp"),
        P(None, "tp"),
        P("tp"),
        P(),
        P("tp", None),
        P(EP_TP, None),
        P(),
        P(EP_TP, None),
        P(EP_TP, None),
        P(EP, None, None),
        P(EP, None, None),
        P(EP, None, None),
        P(None, "tp"),
        P(None, "tp"),
        P("tp", None),
    )
    return jax.shard_map(
        on_device,
        mesh=split,
        in_specs=placed,
        out_specs=(P(EP_TP, None), P(EP_TP, None)),
        check_vma=False,
    )
```

```python
import functools
import math

import jax
import jax.numpy as jnp
from jax import lax
from jax.experimental import pallas as pl
from jax.experimental.pallas import tpu as pltpu
from jax.sharding import Mesh
from jax.sharding import PartitionSpec as P


EP = ("ep_0", "ep_1", "ep_2")
EP_TP = ("ep_0", "ep_1", "ep_2", "tp")
EPS = 1e-06
ROUTED_SCALE = 2.5
LOG2E = 1.4426950408889634
BF = jnp.bfloat16
F32 = jnp.float32
VMEM = pl.BlockSpec(memory_space=pltpu.VMEM)
SMEM = pl.BlockSpec(memory_space=pltpu.SMEM)
HBM = pl.BlockSpec(memory_space=pltpu.MemorySpace.HBM)


def shift(x, axis, k):
    n = lax.axis_size(axis)
    return lax.ppermute(x, axis, [(i, (i + k) % n) for i in range(n)])


def call(kernel, ins, out_shape, flops, nbytes, trans=0, vmem=24, scratch=(), smem_out=()):
    single = not isinstance(out_shape, (list, tuple))
    outs = [out_shape] if single else list(out_shape)
    specs = [SMEM if i in smem_out else VMEM for i in range(len(outs))]
    return pl.pallas_call(
        kernel,
        out_shape=outs[0] if single else outs,
        in_specs=[spec for _, spec in ins],
        out_specs=specs[0] if single else specs,
        scratch_shapes=list(scratch),
        compiler_params=pltpu.CompilerParams(vmem_limit_bytes=vmem * 2**20),
        cost_estimate=pl.CostEstimate(flops=flops, bytes_accessed=nbytes, transcendentals=trans),
    )(*[a for a, _ in ins])


def forward_by_core(fwd, bwd, axis, k):
    n = lax.axis_size(axis)
    picked = jnp.where(lax.axis_index("ep_2") == 0, fwd, bwd)
    last = axis == "tp"
    place = (lambda c, i: c * n + i % n) if last else (lambda c, i: i % n * 2 + c)
    pairs = [(place(c, i), place(c, i + d)) for c, d in ((0, k), (1, -k)) for i in range(n)]
    return lax.ppermute(picked, ("ep_2", axis) if last else (axis, "ep_2"), pairs)


def ring4(x, axis):
    fwd = shift(x, axis, 1)
    bwd = shift(x, axis, -1)
    return x, fwd, bwd, forward_by_core(fwd, bwd, axis, 1)


def rms_rows(matrix, scales):
    values_in = matrix.astype(F32)
    inverse = lax.rsqrt(jnp.mean(values_in * values_in, axis=-1, keepdims=True) + EPS)
    return values_in * inverse * scales


def project_kernel(r0, r1, r2, r3, wq, wk, wv, q_ref, kv_ref):
    rows = jnp.concatenate([r0[...], r1[...], r2[...], r3[...]], axis=0)
    width = wq.shape[1]
    q_ref[...] = jnp.dot(rows, wq[...], preferred_element_type=F32).astype(BF)
    kv_ref[:, :width] = jnp.dot(rows, wk[...], preferred_element_type=F32).astype(BF)
    kv_ref[:, width:] = jnp.dot(rows, wv[...], preferred_element_type=F32).astype(BF)


def silu_product(gate, up):
    return (gate / (1.0 + jnp.exp(-gate)) * up).astype(BF)


def shared_kernel(n, x0, x1, x2, x3, wg, wu, hidden):
    rows = jnp.concatenate([x[:n, :] for x in (x0, x1, x2, x3)], axis=0)
    gate = jnp.dot(rows, wg[...], preferred_element_type=F32)
    up = jnp.dot(rows, wu[...], preferred_element_type=F32)
    hidden[...] = silu_product(gate, up)


def to_tiles(tiles, rows):
    count, subs = rows.shape[0], rows.shape[1] // 128
    for j in range(subs):
        tiles[pl.ds(j, count, stride=subs), :] = rows[:, j * 128 : (j + 1) * 128]


def from_tiles(tiles, out):
    count, subs = out.shape[0], out.shape[1] // 128
    for j in range(subs):
        block = tiles[pl.ds(j, count, stride=subs), :]
        out[:, j * 128 : (j + 1) * 128] = block.astype(out.dtype)


def expert_kernel(x_ref, *refs):
    weights, out, (tiles, rows, wg, wu, wd, hidden, sems) = refs[:3], refs[3], refs[4:]
    step = 256
    halves = hidden.shape[1] // step

    def fetch(i, k):
        cols = pl.ds(pl.multiple_of(i * step, step), step)
        buf = (wg, wu)[k]
        return pltpu.make_async_copy(weights[k].at[0, :, cols], buf.at[:, cols], sems.at[i, k])

    last = pltpu.make_async_copy(weights[2].at[0], wd, sems.at[halves, 0])
    for i in range(halves):
        for k in range(2):
            fetch(i, k).start()
    last.start()
    shape = x_ref.shape
    tiles[...] = x_ref[...].reshape(tiles.shape).astype(F32)
    from_tiles(tiles, rows)

    @pl.loop(0, halves)
    def _(i):
        fetch(i, 0).wait()
        fetch(i, 1).wait()
        cols = pl.ds(pl.multiple_of(i * step, step), step)
        gate = jnp.dot(rows[...], wg[:, cols], preferred_element_type=F32)
        up = jnp.dot(rows[...], wu[:, cols], preferred_element_type=F32)
        hidden[:, cols] = silu_product(gate, up)

    last.wait()
    count, subs = rows.shape[0], rows.shape[1] // 128
    wide = 512

    @pl.loop(0, rows.shape[1] // wide)
    def _(i):
        cols = pl.ds(pl.multiple_of(i * wide, wide), wide)
        part = jnp.dot(hidden[...], wd[:, cols], preferred_element_type=F32)
        for j in range(wide // 128):
            at = pl.ds(i * (wide // 128) + j, count, stride=subs)
            tiles[at, :] = part[:, j * 128 : (j + 1) * 128]

    out[...] = tiles[...].astype(BF).reshape(shape)


def split3(x):
    hi = x.astype(BF)
    rest = x - hi.astype(F32)
    mid = rest.astype(BF)
    low = (rest - mid.astype(F32)).astype(BF)
    return hi, mid, low


def store_lse(ref, rows, lse):
    hi, mid, low = split3(lse)
    ref[rows:, :] = jnp.concatenate(
        [hi.astype(F32), mid.astype(F32), low.astype(F32), jnp.zeros_like(lse)], axis=0
    ).astype(BF)


def load_lse(block):
    b = block.astype(F32)
    return b[0:8] + b[8:16] + b[16:24]


def attend_kernel(half, nq, picks, build, sizes, *refs):
    qs = refs[: 1 + max(i for i, _ in picks)]
    refs = refs[len(qs) :]
    q_all, o_all, s_ref, top_ref, lse_ref = refs[-5:]
    if build:
        kvs, outs, (k_ref, v_ref) = refs[:8], refs[8:-7], refs[-7:-5]
        width = k_ref.shape[1]
        for i, kv in enumerate(kvs):
            n = kv.shape[0]
            k_ref[i * n : (i + 1) * n, :] = kv[:, :width]
            v_ref[i * n : (i + 1) * n, :] = kv[:, width:]
    else:
        (k_ref, v_ref), outs = refs[:2], refs[2:-5]
        width = k_ref.shape[1]
    lane = lax.broadcasted_iota(jnp.int32, (1, width), 1)
    eye = lax.broadcasted_iota(jnp.int32, (128, 128), 0) == lax.broadcasted_iota(
        jnp.int32, (128, 128), 1
    )
    scale = half ** (-0.5)
    count = len(picks)
    for y, (i, side) in enumerate(picks):
        q_all[y * nq : (y + 1) * nq, :] = qs[i][side * nq : (side + 1) * nq, :]
    size = s_ref.shape[1]
    blocks, groups = count * nq // size, size // 128

    def scores(b, c):
        q = q_all[pl.ds(pl.multiple_of(b * size, size), size), :]
        qm = jnp.where((lane // half) == c, q, jnp.zeros_like(q))
        s = lax.dot_general(qm, k_ref[...], (((1,), (1,)), ((), ())), preferred_element_type=F32)
        s_ref[c] = s
        top_ref[c] = jnp.max(s, axis=1, keepdims=True)

    def read(b, c):
        top = top_ref[c]
        p = jnp.exp2((s_ref[c] - top) * (LOG2E * scale))
        total = jnp.sum(p, axis=1, keepdims=True)
        o = jnp.dot(p.astype(BF), v_ref[...], preferred_element_type=F32)
        o_all[c, pl.ds(pl.multiple_of(b * size, size), size), :] = (o / total).astype(BF)
        lse = top * scale + jnp.log(total)
        for g in range(groups):
            row = jnp.where(eye, lse[g * 128 : (g + 1) * 128], 0.0)
            lse_ref[c, b, g : g + 1, :] = jnp.sum(row, axis=0, keepdims=True)

    scores(0, 0)

    @pl.loop(0, blocks)
    def _(b):
        scores(b, 1)
        read(b, 0)
        scores(jnp.minimum(b + 1, blocks - 1), 0)
        read(b, 1)

    parts = nq // 128
    y = 0
    for out, number in zip(outs, sizes):
        for k in range(number):
            ref = out.at[k] if number > 1 else out
            rows = []
            for c in range(2):
                ref[c * nq : (c + 1) * nq, :] = o_all[c, y * nq : (y + 1) * nq, :]
                for g in range(y * parts, (y + 1) * parts):
                    rows.append(lse_ref[c, g // groups, g % groups : g % groups + 1, :])
            rows.append(jnp.zeros((8 - 2 * parts, 128), F32))
            store_lse(ref, 2 * nq, jnp.concatenate(rows, axis=0))
            y += 1


def attend(half, nq, qs, keys_values, picks, groups):
    build = len(keys_values) == 8
    rows, count = 2 * nq + 32, len(picks)
    keys, vdim, block = 8 * nq, 128, math.gcd(256, count * nq)
    S = jax.ShapeDtypeStruct
    outs = [S((n, rows, vdim) if n > 1 else (rows, vdim), BF) for n in groups]
    if build:
        outs += [S((keys, 2 * half), BF), S((keys, vdim), BF)]
    return call(
        functools.partial(attend_kernel, half, nq, picks, build, groups),
        [(q, VMEM) for q in qs] + [(b, VMEM) for b in keys_values],
        outs,
        flops=4 * count * nq * keys * (2 * half + vdim),
        nbytes=4 * 10**6,
        trans=2 * count * nq * keys,
        vmem=24,
        scratch=[
            pltpu.VMEM((count * nq, 2 * half), BF),
            pltpu.VMEM((2, count * nq, vdim), BF),
            pltpu.VMEM((2, block, keys), F32),
            pltpu.VMEM((2, block, 1), F32),
            pltpu.VMEM((2, count * nq // block, 8, 128), F32),
        ],
    )


def row_weights(w, g):
    return jnp.transpose(jnp.broadcast_to(w[g : g + 1, :], (128, 128)))


def merge_cores_kernel(own, rec, o0, o1, o2):
    nrow = own.shape[1] - 32
    for y, out in enumerate((o0, o1, o2)):
        la = load_lse(own[y, nrow:, :])
        lb = load_lse(rec[y, nrow:, :])
        top = jnp.maximum(la, lb)
        wa = jnp.exp(la - top)
        wb = jnp.exp(lb - top)
        total = wa + wb
        fa = wa / total
        fb = wb / total
        for g in range(nrow // 128):
            sl = slice(g * 128, (g + 1) * 128)
            out[sl, :] = (
                row_weights(fa, g) * own[y, sl, :].astype(F32)
                + row_weights(fb, g) * rec[y, sl, :].astype(F32)
            ).astype(BF)
        store_lse(out, nrow, top + jnp.log(total))


def merge_all_kernel(lam, own, rec, p1, p2, p3, gain, hidden, a0, a1, a2, a3, att):
    parts = (own, rec, p1, p2, p3)
    nrow = own.shape[0] - 32
    lses = [load_lse(p[nrow:, :]) for p in parts]
    top = functools.reduce(jnp.maximum, lses)
    ws = [jnp.exp(x - top) for x in lses]
    total = functools.reduce(jnp.add, ws)
    fs = [w / total for w in ws]
    nq = nrow // 2
    lam0 = lam[0]
    for g in range(nq // 128):
        reads = []
        for c in range(2):
            at = c * nq + g * 128
            idx = at // 128
            acc = 0.0
            for f, p in zip(fs, parts):
                acc = acc + row_weights(f, idx) * p[at : at + 128, :].astype(F32)
            reads.append(acc)
        diff = reads[0] - lam0 * reads[1]
        inv = lax.rsqrt(jnp.mean(diff * diff, axis=1, keepdims=True) + EPS)
        att[g * 128 : (g + 1) * 128, :] = (diff * inv * gain[...] * (1.0 - lam0)).astype(BF)
    n = nq // 4
    for i, a in enumerate((a0, a1, a2, a3)):
        a[:n, :] = att[i * n : (i + 1) * n, :]
        a[n:, :] = hidden[i * n : (i + 1) * n, :]


def project_out_kernel(n, a0, a1, a2, a3, wo, wd, x1, x2, x3, routed, mixed, expert):
    depth = wo.shape[0]
    for i, (own, extra, out) in enumerate(((wo, None, mixed), (wd, routed, expert))):
        lo, hi = n + i * depth, n + (i + 1) * depth
        total = None if extra is None else extra[...]
        for a, w in zip((a0, a1, a2, a3), (own, x2, x1, x3)):
            rows = w[...] if w is own else w[lo:hi, :]
            part = jnp.dot(a[i * n : (i + 1) * n, :], rows, preferred_element_type=F32)
            part = part.astype(BF).astype(F32)
            total = part if total is None else total + part
        out[...] = total.astype(out.dtype)


def dispatch_kernel(capacity, top_count, x_ref, gain, routes, out, normed, slots, tiles, xf, count):
    x = x_ref[...].astype(F32)
    inverse = lax.rsqrt(jnp.mean(x * x, axis=1, keepdims=True) + EPS)
    x = x * inverse * gain[...]
    normed[...] = x.astype(BF)
    to_tiles(tiles, x)
    xf[...] = tiles[...].astype(BF).reshape(xf.shape)
    out[...] = jnp.zeros_like(out)
    for e in range(count.shape[0]):
        count[e] = 0

    def step(t, carry):
        row = xf[t]
        for k in range(top_count):
            i = t * top_count + k
            e = routes[i]
            c = count[e]
            count[e] = c + 1
            s = e * capacity + c
            slots[i] = s
            out[s] = row
        return carry

    lax.fori_loop(0, x_ref.shape[0], step, 0)


def combine_kernel(top_count, ret, slots, shares, out, tiles):
    subs = ret.shape[1]

    def step(t, carry):
        acc = None
        for k in range(top_count):
            i = t * top_count + k
            v = ret[slots[i]].astype(F32) * shares[i]
            acc = v if acc is None else acc + v
        tiles[pl.ds(pl.multiple_of(t * subs, subs), subs), :] = acc
        return carry

    lax.fori_loop(0, out.shape[0], step, 0)
    from_tiles(tiles, out)


def on_device(
    mixer_in,
    mixer_gain,
    query_weight,
    key_weight,
    value_weight,
    head_lambda,
    head_gain,
    out_weight,
    expert_in,
    expert_gain,
    routes,
    route_weights,
    gate_weight,
    up_weight,
    down_weight,
    shared_gate,
    shared_up,
    shared_down,
):
    tokens, width = mixer_in.shape
    vdim = head_gain.shape[0]
    half = query_weight.shape[1] // 2
    nq = 4 * tokens
    experts = lax.axis_size(EP)
    top_count = routes.shape[1]
    capacity = 2 * tokens * top_count // experts
    slots_all = experts * capacity
    lanes = 128
    subs = width // lanes
    S = jax.ShapeDtypeStruct

    normed_mixer = rms_rows(mixer_in, mixer_gain).astype(BF)
    mixer_rows = ring4(normed_mixer, "tp")
    queries, kv = call(
        project_kernel,
        [(r, VMEM) for r in mixer_rows]
        + [(query_weight, VMEM), (key_weight, VMEM), (value_weight, VMEM)],
        [S((nq, 2 * half), BF), S((nq, 2 * half + vdim), BF)],
        flops=2 * nq * width * (4 * half + vdim),
        nbytes=4 * 10**6,
        vmem=12,
    )

    flat_routes = routes.reshape(-1)
    outgoing, normed_expert, slot_index = call(
        functools.partial(dispatch_kernel, capacity, top_count),
        [
            (expert_in, VMEM),
            (expert_gain.reshape(1, width), VMEM),
            (flat_routes, SMEM),
        ],
        [
            S((slots_all, subs, lanes), BF),
            S((tokens, width), BF),
            S((tokens * top_count,), jnp.int32),
        ],
        flops=10**7,
        nbytes=2 * 10**6,
        scratch=[
            pltpu.VMEM((tokens * subs, lanes), F32),
            pltpu.VMEM((tokens, subs, lanes), BF),
            pltpu.SMEM((experts,), jnp.int32),
        ],
        smem_out=(2,),
        vmem=12,
    )
    arrived = lax.all_to_all(
        outgoing.reshape(experts, capacity * subs, lanes), EP, 0, 0, tiled=True
    )

    shares = ROUTED_SCALE * route_weights / jnp.sum(route_weights, axis=1, keepdims=True)
    queries, shares = lax.optimization_barrier((queries, shares.reshape(-1)))

    near = [shift(kv, "ep_0", k) for k in (1, -1, 2, -2)]
    far = [shift(near[2], "ep_0", 1), shift(near[3], "ep_0", -1)]
    far.append(shift(near[3], "ep_0", -2))
    kvs = [kv] + near + far
    q_pair = jnp.concatenate([queries, shift(queries, "ep_2", 1)], axis=0)
    q_all = [q_pair] + [shift(q_pair, "ep_1", k) for k in (1, -1, 2)]

    normed_expert, _ = lax.optimization_barrier((normed_expert, mixer_rows[1]))
    joined = jnp.concatenate([normed_expert, out_weight, shared_down], axis=0)
    tails = ring4(joined, "tp")
    hidden = call(
        functools.partial(shared_kernel, tokens),
        [(r, VMEM) for r in tails] + [(shared_gate, VMEM), (shared_up, VMEM)],
        S((nq, vdim), BF),
        flops=4 * nq * width * vdim,
        nbytes=3 * 10**6,
        vmem=12,
    )

    result = call(
        expert_kernel,
        [
            (arrived.reshape(slots_all, subs, lanes), VMEM),
            (gate_weight, HBM),
            (up_weight, HBM),
            (down_weight, HBM),
        ],
        S((slots_all, subs, lanes), BF),
        flops=6 * slots_all * width * gate_weight.shape[2],
        nbytes=10 * 10**6,
        scratch=[
            pltpu.VMEM((slots_all * subs, lanes), F32),
            pltpu.VMEM((slots_all, width), BF),
            pltpu.VMEM(gate_weight.shape[1:], BF),
            pltpu.VMEM(up_weight.shape[1:], BF),
            pltpu.VMEM(down_weight.shape[1:], BF),
            pltpu.VMEM((slots_all, gate_weight.shape[2]), BF),
            pltpu.SemaphoreType.DMA((gate_weight.shape[2] // 256 + 1, 2)),
        ],
        vmem=54,
    )
    returned = lax.all_to_all(result.reshape(experts, capacity * subs, lanes), EP, 0, 0, tiled=True)

    sides = tuple((i, side) for side in (1, 0) for i in (1, 2, 3))
    peer, own, keys_all, values_all = attend(half, nq, q_all, kvs, sides, (3, 3))
    received = shift(peer, "ep_2", 1)
    peer0, own0 = attend(half, nq, q_all[:1], [keys_all, values_all], ((0, 1), (0, 0)), (1, 1))
    merged = call(
        merge_cores_kernel,
        [(own, VMEM), (received, VMEM)],
        [S((2 * nq + 32, vdim), BF)] * 3,
        flops=5 * 10**7,
        nbytes=3 * 10**6,
        vmem=8,
    )
    parts = [own0, shift(peer0, "ep_2", 1)]
    for i, k in enumerate((-1, 1, 2)):
        parts.append(shift(merged[i], "ep_1", k))
    attended = call(
        merge_all_kernel,
        [(head_lambda, SMEM)]
        + [(p, VMEM) for p in parts]
        + [(head_gain.reshape(1, vdim), VMEM)]
        + [(hidden, VMEM)],
        [S((2 * tokens, vdim), BF)] * 4,
        flops=5 * 10**7,
        nbytes=10**6,
        scratch=[pltpu.VMEM((nq, vdim), BF)],
        vmem=8,
    )
    backs = [attended[0]]
    for i, k in enumerate((-1, 1, 2)):
        backs.append(shift(attended[i + 1], "tp", k))
    routed = call(
        functools.partial(combine_kernel, top_count),
        [
            (returned.reshape(slots_all, subs, lanes), VMEM),
            (slot_index, SMEM),
            (shares, SMEM),
        ],
        S((tokens, width), F32),
        flops=10**7,
        nbytes=3 * 10**6,
        scratch=[pltpu.VMEM((tokens * subs, lanes), F32)],
        vmem=8,
    )
    mixed_out, expert_out = call(
        functools.partial(project_out_kernel, tokens),
        [(a, VMEM) for a in backs]
        + [(out_weight, VMEM), (shared_down, VMEM)]
        + [(w, VMEM) for w in tails[1:]]
        + [(routed, VMEM)],
        [S((tokens, width), BF), S((tokens, width), BF)],
        flops=16 * tokens * vdim * width,
        nbytes=8 * 10**6,
        vmem=12,
    )

    return (mixed_out, expert_out)


def solution(mesh):
    split = Mesh(mesh.devices.reshape(8, 4, 2, mesh.shape["tp"]), ("ep_0", "ep_1", "ep_2", "tp"))
    placed = (
        P(EP_TP, None),
        P(),
        P(None, "tp"),
        P(None, "tp"),
        P(None, "tp"),
        P("tp"),
        P(),
        P("tp", None),
        P(EP_TP, None),
        P(),
        P(EP_TP, None),
        P(EP_TP, None),
        P(EP, None, None),
        P(EP, None, None),
        P(EP, None, None),
        P(None, "tp"),
        P(None, "tp"),
        P("tp", None),
    )
    return jax.shard_map(
        on_device,
        mesh=split,
        in_specs=placed,
        out_specs=(P(EP_TP, None), P(EP_TP, None)),
        check_vma=False,
    )
```

```python
import functools
import math

import jax
import jax.numpy as jnp
from jax import lax
from jax.experimental import pallas as pl
from jax.experimental.pallas import tpu as pltpu
from jax.sharding import Mesh
from jax.sharding import PartitionSpec as P


EP = ("ep_0", "ep_1", "ep_2")
EP_TP = ("ep_0", "ep_1", "ep_2", "tp")
EPS = 1e-06
ROUTED_SCALE = 2.5
LOG2E = 1.4426950408889634
BF = jnp.bfloat16
F32 = jnp.float32
VMEM = pl.BlockSpec(memory_space=pltpu.VMEM)
SMEM = pl.BlockSpec(memory_space=pltpu.SMEM)
HBM = pl.BlockSpec(memory_space=pltpu.MemorySpace.HBM)


def shift(x, axis, k):
    n = lax.axis_size(axis)
    return lax.ppermute(x, axis, [(i, (i + k) % n) for i in range(n)])


def call(kernel, ins, out_shape, flops, nbytes, trans=0, vmem=24, scratch=(), smem_out=()):
    single = not isinstance(out_shape, (list, tuple))
    outs = [out_shape] if single else list(out_shape)
    specs = [SMEM if i in smem_out else VMEM for i in range(len(outs))]
    return pl.pallas_call(
        kernel,
        out_shape=outs[0] if single else outs,
        in_specs=[spec for _, spec in ins],
        out_specs=specs[0] if single else specs,
        scratch_shapes=list(scratch),
        compiler_params=pltpu.CompilerParams(vmem_limit_bytes=vmem * 2**20),
        cost_estimate=pl.CostEstimate(flops=flops, bytes_accessed=nbytes, transcendentals=trans),
    )(*[a for a, _ in ins])


def forward_by_core(fwd, bwd, axis, k):
    n = lax.axis_size(axis)
    picked = jnp.where(lax.axis_index("ep_2") == 0, fwd, bwd)
    last = axis == "tp"
    place = (lambda c, i: c * n + i % n) if last else (lambda c, i: i % n * 2 + c)
    pairs = [(place(c, i), place(c, i + d)) for c, d in ((0, k), (1, -k)) for i in range(n)]
    return lax.ppermute(picked, ("ep_2", axis) if last else (axis, "ep_2"), pairs)


def ring4(x, axis):
    fwd = shift(x, axis, 1)
    bwd = shift(x, axis, -1)
    return x, fwd, bwd, forward_by_core(fwd, bwd, axis, 1)


def rms_rows(matrix, scales):
    values_in = matrix.astype(F32)
    inverse = lax.rsqrt(jnp.mean(values_in * values_in, axis=-1, keepdims=True) + EPS)
    return values_in * inverse * scales


def project_kernel(r0, r1, r2, r3, wq, wk, wv, q_ref, kv_ref):
    rows = jnp.concatenate([r0[...], r1[...], r2[...], r3[...]], axis=0)
    width = wq.shape[1]
    q_ref[...] = jnp.dot(rows, wq[...], preferred_element_type=F32).astype(BF)
    kv_ref[:, :width] = jnp.dot(rows, wk[...], preferred_element_type=F32).astype(BF)
    kv_ref[:, width:] = jnp.dot(rows, wv[...], preferred_element_type=F32).astype(BF)


def silu_product(gate, up):
    return (gate / (1.0 + jnp.exp(-gate)) * up).astype(BF)


def shared_kernel(n, x0, x1, x2, x3, wg, wu, hidden):
    rows = jnp.concatenate([x[:n, :] for x in (x0, x1, x2, x3)], axis=0)
    gate = jnp.dot(rows, wg[...], preferred_element_type=F32)
    up = jnp.dot(rows, wu[...], preferred_element_type=F32)
    hidden[...] = silu_product(gate, up)


def to_tiles(tiles, rows):
    count, subs = rows.shape[0], rows.shape[1] // 128
    for j in range(subs):
        tiles[pl.ds(j, count, stride=subs), :] = rows[:, j * 128 : (j + 1) * 128]


def from_tiles(tiles, out):
    count, subs = out.shape[0], out.shape[1] // 128
    for j in range(subs):
        block = tiles[pl.ds(j, count, stride=subs), :]
        out[:, j * 128 : (j + 1) * 128] = block.astype(out.dtype)


def expert_kernel(x_ref, *refs):
    weights, out, (tiles, rows, wg, wu, wd, hidden, sems) = refs[:3], refs[3], refs[4:]
    step = 256
    halves = hidden.shape[1] // step

    def fetch(i, k):
        cols = pl.ds(pl.multiple_of(i * step, step), step)
        buf = (wg, wu)[k]
        return pltpu.make_async_copy(weights[k].at[0, :, cols], buf.at[:, cols], sems.at[i, k])

    last = pltpu.make_async_copy(weights[2].at[0], wd, sems.at[halves, 0])
    for i in range(halves):
        for k in range(2):
            fetch(i, k).start()
    last.start()
    shape = x_ref.shape
    tiles[...] = x_ref[...].reshape(tiles.shape).astype(F32)
    from_tiles(tiles, rows)

    @pl.loop(0, halves)
    def _(i):
        fetch(i, 0).wait()
        fetch(i, 1).wait()
        cols = pl.ds(pl.multiple_of(i * step, step), step)
        gate = jnp.dot(rows[...], wg[:, cols], preferred_element_type=F32)
        up = jnp.dot(rows[...], wu[:, cols], preferred_element_type=F32)
        hidden[:, cols] = silu_product(gate, up)

    last.wait()
    count, subs = rows.shape[0], rows.shape[1] // 128
    wide = 512

    @pl.loop(0, rows.shape[1] // wide)
    def _(i):
        cols = pl.ds(pl.multiple_of(i * wide, wide), wide)
        part = jnp.dot(hidden[...], wd[:, cols], preferred_element_type=F32)
        for j in range(wide // 128):
            at = pl.ds(i * (wide // 128) + j, count, stride=subs)
            tiles[at, :] = part[:, j * 128 : (j + 1) * 128]

    out[...] = tiles[...].astype(BF).reshape(shape)


def split3(x):
    hi = x.astype(BF)
    rest = x - hi.astype(F32)
    mid = rest.astype(BF)
    low = (rest - mid.astype(F32)).astype(BF)
    return hi, mid, low


def store_lse(ref, rows, lse):
    hi, mid, low = split3(lse)
    ref[rows:, :] = jnp.concatenate(
        [hi.astype(F32), mid.astype(F32), low.astype(F32), jnp.zeros_like(lse)], axis=0
    ).astype(BF)


def load_lse(block):
    b = block.astype(F32)
    return b[0:8] + b[8:16] + b[16:24]


def attend_kernel(half, nq, picks, build, sizes, *refs):
    qs = refs[: 1 + max(i for i, _ in picks)]
    refs = refs[len(qs) :]
    q_all, o_all, s_ref, top_ref, lse_ref = refs[-5:]
    if build:
        kvs, outs, (k_ref, v_ref) = refs[:8], refs[8:-7], refs[-7:-5]
        width = k_ref.shape[1]
        for i, kv in enumerate(kvs):
            n = kv.shape[0]
            k_ref[i * n : (i + 1) * n, :] = kv[:, :width]
            v_ref[i * n : (i + 1) * n, :] = kv[:, width:]
    else:
        (k_ref, v_ref), outs = refs[:2], refs[2:-5]
        width = k_ref.shape[1]
    lane = lax.broadcasted_iota(jnp.int32, (1, width), 1)
    eye = lax.broadcasted_iota(jnp.int32, (128, 128), 0) == lax.broadcasted_iota(
        jnp.int32, (128, 128), 1
    )
    scale = half ** (-0.5)
    count = len(picks)
    for y, (i, side) in enumerate(picks):
        q_all[y * nq : (y + 1) * nq, :] = qs[i][side * nq : (side + 1) * nq, :]
    size = s_ref.shape[1]
    blocks, groups = count * nq // size, size // 128

    def scores(b, c):
        q = q_all[pl.ds(pl.multiple_of(b * size, size), size), :]
        qm = jnp.where((lane // half) == c, q, jnp.zeros_like(q))
        s = lax.dot_general(qm, k_ref[...], (((1,), (1,)), ((), ())), preferred_element_type=F32)
        s_ref[c] = s
        top_ref[c] = jnp.max(s, axis=1, keepdims=True)

    def read(b, c):
        top = top_ref[c]
        p = jnp.exp2((s_ref[c] - top) * (LOG2E * scale))
        total = jnp.sum(p, axis=1, keepdims=True)
        o = jnp.dot(p.astype(BF), v_ref[...], preferred_element_type=F32)
        o_all[c, pl.ds(pl.multiple_of(b * size, size), size), :] = (o / total).astype(BF)
        lse = top * scale + jnp.log(total)
        for g in range(groups):
            row = jnp.where(eye, lse[g * 128 : (g + 1) * 128], 0.0)
            lse_ref[c, b, g : g + 1, :] = jnp.sum(row, axis=0, keepdims=True)

    scores(0, 0)

    @pl.loop(0, blocks)
    def _(b):
        scores(b, 1)
        read(b, 0)
        scores(jnp.minimum(b + 1, blocks - 1), 0)
        read(b, 1)

    parts = nq // 128
    y = 0
    for out, number in zip(outs, sizes):
        for k in range(number):
            ref = out.at[k] if number > 1 else out
            rows = []
            for c in range(2):
                ref[c * nq : (c + 1) * nq, :] = o_all[c, y * nq : (y + 1) * nq, :]
                for g in range(y * parts, (y + 1) * parts):
                    rows.append(lse_ref[c, g // groups, g % groups : g % groups + 1, :])
            rows.append(jnp.zeros((8 - 2 * parts, 128), F32))
            store_lse(ref, 2 * nq, jnp.concatenate(rows, axis=0))
            y += 1


def attend(half, nq, qs, keys_values, picks, groups):
    build = len(keys_values) == 8
    rows, count = 2 * nq + 32, len(picks)
    keys, vdim, block = 8 * nq, 128, math.gcd(256, count * nq)
    S = jax.ShapeDtypeStruct
    outs = [S((n, rows, vdim) if n > 1 else (rows, vdim), BF) for n in groups]
    if build:
        outs += [S((keys, 2 * half), BF), S((keys, vdim), BF)]
    return call(
        functools.partial(attend_kernel, half, nq, picks, build, groups),
        [(q, VMEM) for q in qs] + [(b, VMEM) for b in keys_values],
        outs,
        flops=4 * count * nq * keys * (2 * half + vdim),
        nbytes=4 * 10**6,
        trans=2 * count * nq * keys,
        vmem=24,
        scratch=[
            pltpu.VMEM((count * nq, 2 * half), BF),
            pltpu.VMEM((2, count * nq, vdim), BF),
            pltpu.VMEM((2, block, keys), F32),
            pltpu.VMEM((2, block, 1), F32),
            pltpu.VMEM((2, count * nq // block, 8, 128), F32),
        ],
    )


def row_weights(w, g):
    return jnp.transpose(jnp.broadcast_to(w[g : g + 1, :], (128, 128)))


def merge_cores_kernel(own, rec, o0, o1, o2):
    nrow = own.shape[1] - 32
    for y, out in enumerate((o0, o1, o2)):
        la = load_lse(own[y, nrow:, :])
        lb = load_lse(rec[y, nrow:, :])
        top = jnp.maximum(la, lb)
        wa = jnp.exp(la - top)
        wb = jnp.exp(lb - top)
        total = wa + wb
        fa = wa / total
        fb = wb / total
        for g in range(nrow // 128):
            sl = slice(g * 128, (g + 1) * 128)
            out[sl, :] = (
                row_weights(fa, g) * own[y, sl, :].astype(F32)
                + row_weights(fb, g) * rec[y, sl, :].astype(F32)
            ).astype(BF)
        store_lse(out, nrow, top + jnp.log(total))


def merge_all_kernel(lam, own, rec, p1, p2, p3, gain, hidden, a0, a1, a2, a3, att):
    parts = (own, rec, p1, p2, p3)
    nrow = own.shape[0] - 32
    lses = [load_lse(p[nrow:, :]) for p in parts]
    top = functools.reduce(jnp.maximum, lses)
    ws = [jnp.exp(x - top) for x in lses]
    total = functools.reduce(jnp.add, ws)
    fs = [w / total for w in ws]
    nq = nrow // 2
    lam0 = lam[0]
    for g in range(nq // 128):
        reads = []
        for c in range(2):
            at = c * nq + g * 128
            idx = at // 128
            acc = 0.0
            for f, p in zip(fs, parts):
                acc = acc + row_weights(f, idx) * p[at : at + 128, :].astype(F32)
            reads.append(acc)
        diff = reads[0] - lam0 * reads[1]
        inv = lax.rsqrt(jnp.mean(diff * diff, axis=1, keepdims=True) + EPS)
        att[g * 128 : (g + 1) * 128, :] = (diff * inv * gain[...] * (1.0 - lam0)).astype(BF)
    n = nq // 4
    for i, a in enumerate((a0, a1, a2, a3)):
        a[:n, :] = att[i * n : (i + 1) * n, :]
        a[n:, :] = hidden[i * n : (i + 1) * n, :]


def project_out_kernel(n, a0, a1, a2, a3, wo, wd, x1, x2, x3, routed, mixed, expert):
    depth = wo.shape[0]
    for i, (own, extra, out) in enumerate(((wo, None, mixed), (wd, routed, expert))):
        lo, hi = n + i * depth, n + (i + 1) * depth
        total = None if extra is None else extra[...]
        for a, w in zip((a0, a1, a2, a3), (own, x2, x1, x3)):
            rows = w[...] if w is own else w[lo:hi, :]
            part = jnp.dot(a[i * n : (i + 1) * n, :], rows, preferred_element_type=F32)
            part = part.astype(BF).astype(F32)
            total = part if total is None else total + part
        out[...] = total.astype(out.dtype)


def dispatch_kernel(capacity, top_count, x_ref, gain, routes, out, normed, slots, tiles, xf, count):
    x = x_ref[...].astype(F32)
    inverse = lax.rsqrt(jnp.mean(x * x, axis=1, keepdims=True) + EPS)
    x = x * inverse * gain[...]
    normed[...] = x.astype(BF)
    to_tiles(tiles, x)
    xf[...] = tiles[...].astype(BF).reshape(xf.shape)
    out[...] = jnp.zeros_like(out)
    for e in range(count.shape[0]):
        count[e] = 0

    def step(t, carry):
        row = xf[t]
        for k in range(top_count):
            i = t * top_count + k
            e = routes[k, t]
            c = count[e]
            count[e] = c + 1
            s = e * capacity + c
            slots[i] = s
            out[s] = row
        return carry

    lax.fori_loop(0, x_ref.shape[0], step, 0, unroll=4)


def combine_kernel(top_count, ret, slots, shares, out, tiles):
    subs = ret.shape[1]

    def step(t, carry):
        acc = None
        for k in range(top_count):
            i = t * top_count + k
            v = ret[slots[i]].astype(F32) * shares[k, t]
            acc = v if acc is None else acc + v
        tiles[pl.ds(pl.multiple_of(t * subs, subs), subs), :] = acc
        return carry

    lax.fori_loop(0, out.shape[0], step, 0, unroll=4)
    from_tiles(tiles, out)


def on_device(
    mixer_in,
    mixer_gain,
    query_weight,
    key_weight,
    value_weight,
    head_lambda,
    head_gain,
    out_weight,
    expert_in,
    expert_gain,
    routes,
    route_weights,
    gate_weight,
    up_weight,
    down_weight,
    shared_gate,
    shared_up,
    shared_down,
):
    tokens, width = mixer_in.shape
    vdim = head_gain.shape[0]
    half = query_weight.shape[1] // 2
    nq = 4 * tokens
    experts = lax.axis_size(EP)
    top_count = routes.shape[1]
    capacity = 2 * tokens * top_count // experts
    slots_all = experts * capacity
    lanes = 128
    subs = width // lanes
    S = jax.ShapeDtypeStruct

    normed_mixer = rms_rows(mixer_in, mixer_gain).astype(BF)
    mixer_rows = ring4(normed_mixer, "tp")
    queries, kv = call(
        project_kernel,
        [(r, VMEM) for r in mixer_rows]
        + [(query_weight, VMEM), (key_weight, VMEM), (value_weight, VMEM)],
        [S((nq, 2 * half), BF), S((nq, 2 * half + vdim), BF)],
        flops=2 * nq * width * (4 * half + vdim),
        nbytes=4 * 10**6,
        vmem=12,
    )

    outgoing, normed_expert, slot_index = call(
        functools.partial(dispatch_kernel, capacity, top_count),
        [
            (expert_in, VMEM),
            (expert_gain.reshape(1, width), VMEM),
            (routes.T, SMEM),
        ],
        [
            S((slots_all, subs, lanes), BF),
            S((tokens, width), BF),
            S((tokens * top_count,), jnp.int32),
        ],
        flops=10**7,
        nbytes=2 * 10**6,
        scratch=[
            pltpu.VMEM((tokens * subs, lanes), F32),
            pltpu.VMEM((tokens, subs, lanes), BF),
            pltpu.SMEM((experts,), jnp.int32),
        ],
        smem_out=(2,),
        vmem=12,
    )
    arrived = lax.all_to_all(
        outgoing.reshape(experts, capacity * subs, lanes), EP, 0, 0, tiled=True
    )

    shares = ROUTED_SCALE * route_weights / jnp.sum(route_weights, axis=1, keepdims=True)
    queries, shares = lax.optimization_barrier((queries, shares.T))

    near = [shift(kv, "ep_0", k) for k in (1, -1, 2, -2)]
    far = [shift(near[2], "ep_0", 1), shift(near[3], "ep_0", -1)]
    far.append(shift(near[3], "ep_0", -2))
    kvs = [kv] + near + far
    q_pair = jnp.concatenate([queries, shift(queries, "ep_2", 1)], axis=0)
    q_all = [q_pair] + [shift(q_pair, "ep_1", k) for k in (1, -1, 2)]

    normed_expert, _ = lax.optimization_barrier((normed_expert, mixer_rows[1]))
    joined = jnp.concatenate([normed_expert, out_weight, shared_down], axis=0)
    tails = ring4(joined, "tp")
    hidden = call(
        functools.partial(shared_kernel, tokens),
        [(r, VMEM) for r in tails] + [(shared_gate, VMEM), (shared_up, VMEM)],
        S((nq, vdim), BF),
        flops=4 * nq * width * vdim,
        nbytes=3 * 10**6,
        vmem=12,
    )

    result = call(
        expert_kernel,
        [
            (arrived.reshape(slots_all, subs, lanes), VMEM),
            (gate_weight, HBM),
            (up_weight, HBM),
            (down_weight, HBM),
        ],
        S((slots_all, subs, lanes), BF),
        flops=6 * slots_all * width * gate_weight.shape[2],
        nbytes=10 * 10**6,
        scratch=[
            pltpu.VMEM((slots_all * subs, lanes), F32),
            pltpu.VMEM((slots_all, width), BF),
            pltpu.VMEM(gate_weight.shape[1:], BF),
            pltpu.VMEM(up_weight.shape[1:], BF),
            pltpu.VMEM(down_weight.shape[1:], BF),
            pltpu.VMEM((slots_all, gate_weight.shape[2]), BF),
            pltpu.SemaphoreType.DMA((gate_weight.shape[2] // 256 + 1, 2)),
        ],
        vmem=54,
    )
    returned = lax.all_to_all(result.reshape(experts, capacity * subs, lanes), EP, 0, 0, tiled=True)

    sides = tuple((i, side) for side in (1, 0) for i in (1, 2, 3))
    peer, own, keys_all, values_all = attend(half, nq, q_all, kvs, sides, (3, 3))
    received = shift(peer, "ep_2", 1)
    peer0, own0 = attend(half, nq, q_all[:1], [keys_all, values_all], ((0, 1), (0, 0)), (1, 1))
    merged = call(
        merge_cores_kernel,
        [(own, VMEM), (received, VMEM)],
        [S((2 * nq + 32, vdim), BF)] * 3,
        flops=5 * 10**7,
        nbytes=3 * 10**6,
        vmem=8,
    )
    parts = [own0, shift(peer0, "ep_2", 1)]
    for i, k in enumerate((-1, 1, 2)):
        parts.append(shift(merged[i], "ep_1", k))
    attended = call(
        merge_all_kernel,
        [(head_lambda, SMEM)]
        + [(p, VMEM) for p in parts]
        + [(head_gain.reshape(1, vdim), VMEM)]
        + [(hidden, VMEM)],
        [S((2 * tokens, vdim), BF)] * 4,
        flops=5 * 10**7,
        nbytes=10**6,
        scratch=[pltpu.VMEM((nq, vdim), BF)],
        vmem=8,
    )
    backs = [attended[0]]
    for i, k in enumerate((-1, 1, 2)):
        backs.append(shift(attended[i + 1], "tp", k))
    routed = call(
        functools.partial(combine_kernel, top_count),
        [
            (returned.reshape(slots_all, subs, lanes), VMEM),
            (slot_index, SMEM),
            (shares, SMEM),
        ],
        S((tokens, width), F32),
        flops=10**7,
        nbytes=3 * 10**6,
        scratch=[pltpu.VMEM((tokens * subs, lanes), F32)],
        vmem=8,
    )
    mixed_out, expert_out = call(
        functools.partial(project_out_kernel, tokens),
        [(a, VMEM) for a in backs]
        + [(out_weight, VMEM), (shared_down, VMEM)]
        + [(w, VMEM) for w in tails[1:]]
        + [(routed, VMEM)],
        [S((tokens, width), BF), S((tokens, width), BF)],
        flops=16 * tokens * vdim * width,
        nbytes=8 * 10**6,
        vmem=12,
    )

    return (mixed_out, expert_out)


def solution(mesh):
    split = Mesh(mesh.devices.reshape(8, 4, 2, mesh.shape["tp"]), ("ep_0", "ep_1", "ep_2", "tp"))
    placed = (
        P(EP_TP, None),
        P(),
        P(None, "tp"),
        P(None, "tp"),
        P(None, "tp"),
        P("tp"),
        P(),
        P("tp", None),
        P(EP_TP, None),
        P(),
        P(EP_TP, None),
        P(EP_TP, None),
        P(EP, None, None),
        P(EP, None, None),
        P(EP, None, None),
        P(None, "tp"),
        P(None, "tp"),
        P("tp", None),
    )
    return jax.shard_map(
        on_device,
        mesh=split,
        in_specs=placed,
        out_specs=(P(EP_TP, None), P(EP_TP, None)),
        check_vma=False,
    )
```
